32 devices in a mesh: rep: 4 (over z), fs: 2 (over y), tp: 4 (over x, core).
Axes of the slice: x: 2, y: 2, z: 4, core: 2. Of those that a mesh axis runs over, the one named last changes fastest.
Arguments:
- tokens: bfloat16 [3072, 2048], P('rep', 'fs'), may hold values from -6 to 6
- gate_pre: bfloat16 [3072, 6144], P('rep', 'tp'), may hold values from -6 to 6
- up_pre: bfloat16 [3072, 6144], P('rep', 'tp'), may hold values from -6 to 6
- hidden_grad: bfloat16 [3072, 6144], P('rep', 'tp'), may hold values from -0.75 to 0.75
- gate_weight: bfloat16 [2048, 6144], P('fs', 'tp'), may hold values from -0.125 to 0.125
- up_weight: bfloat16 [2048, 6144], P('fs', 'tp'), may hold values from -0.125 to 0.125
- gate_taps: float32 [3, 6144], P(None, 'tp'), may hold values from -3.5 to 3.5
- up_taps: float32 [3, 6144], P(None, 'tp'), may hold values from -3.5 to 3.5
- gate_bias: float32 [6144], P('tp'), may hold values from -4 to 4
- up_bias: float32 [6144], P('tp'), may hold values from -4 to 4
Outputs:
- input_grad: bfloat16 [3072, 2048], P('rep', 'fs')
- gate_weight_grad: float32 [2048, 6144], P('fs', 'tp')
- up_weight_grad: float32 [2048, 6144], P('fs', 'tp')
- gate_taps_grad: float32 [3, 6144], P(None, 'tp')
- up_taps_grad: float32 [3, 6144], P(None, 'tp')
- gate_bias_grad: float32 [6144], P('tp')
- up_bias_grad: float32 [6144], P('tp')
The draws below stay inside these ranges and needn't reach their ends.
All inputs are finite; a program needn't handle non-finite values.
Results may differ from the reference program's by a relative error of at most 0.017.
Values may be sent and summed in bfloat16 or wider, within the bound.
A program may use at most 64 MiB of HBM per device.

```python
import jax
import jax.numpy as jnp
from jax import lax

D = 2048
FF = 6144
TAPS = 3
SEQ_LEN = 768
TOKENS = 3072
N_REP = 4
N_TP = 4


def strengthened(entries, stream_key, source, target, blocks, factor):
    def block_of(dim):
        return (jnp.arange(entries.shape[dim]) // (entries.shape[dim] // blocks)).reshape((-1,) + (1,) * (entries.ndim - 1 - dim))

    near = jax.random.permutation(stream_key, blocks)[block_of(target)]
    second = (block_of(target) + blocks // 2) % blocks
    return jnp.where((block_of(source) == near) | (block_of(source) == second), factor * entries, entries)


def level_of(own_key, shape, split, low, high):
    gain = 1.0
    for position, blocks in split:
        draws = jax.random.uniform(jax.random.fold_in(jax.random.fold_in(own_key, 6), position), (blocks,), jnp.float32, low / len(split), high / len(split))
        gain = gain * jnp.repeat(jnp.exp(draws), shape[position] // blocks).reshape((-1,) + (1,) * (len(shape) - 1 - position))
    return gain


def noise(own_key, dims, width, most, split=(), kind=jnp.bfloat16):
    gain = level_of(own_key, dims, split, -0.22, 0.18) if split else 1.0
    values = jax.random.normal(own_key, dims, jnp.float32) * width * gain
    return jnp.minimum(jnp.maximum(values, -most), most).astype(kind)


def bell_draw_with(stream_key, dims, spread, bound, split, heavy, held_as=jnp.bfloat16):
    array = spread * jax.random.normal(stream_key, dims, jnp.float32)
    if split:
        array = array * level_of(stream_key, dims, split, -0.22, 0.18)
    return jnp.clip(strengthened(array, jax.random.fold_in(stream_key, 3), *heavy), -bound, bound).astype(held_as)


def setup_inputs(seed: int = 0) -> dict:
    key_list = jax.random.split(jax.random.key(seed), 11)
    tokens = noise(key_list[0], (TOKENS, D), 1.0, 6.0, ((0, 4), (1, 2)))
    gate_pre = noise(key_list[1], (TOKENS, FF), 1.0, 6.0, ((0, 4), (1, 4)))
    up_pre = noise(key_list[2], (TOKENS, FF), 1.0, 6.0, ((0, 4), (1, 4)))
    hidden_grad = bell_draw_with(key_list[3], (TOKENS, FF), 0.125, 0.75, ((0, 4), (1, 4)), (1, 0, 4, 2.0))
    gate_weight = noise(key_list[4], (D, FF), D ** -0.5, 0.125, ((0, 2), (1, 4)))
    up_weight = noise(key_list[5], (D, FF), D ** -0.5, 0.125, ((0, 2), (1, 4)))
    gate_taps = noise(key_list[6], (TAPS, FF), TAPS ** -0.5, 3.5, ((1, 4),), jnp.float32)
    up_taps = noise(key_list[7], (TAPS, FF), TAPS ** -0.5, 3.5, ((1, 4),), jnp.float32)
    gate_bias = noise(key_list[8], (FF,), 1.0, 4.0, ((0, 4),), jnp.float32)
    up_bias = noise(key_list[9], (FF,), 1.0, 4.0, ((0, 4),), jnp.float32)
    return dict(tokens=tokens, gate_pre=gate_pre, up_pre=up_pre, hidden_grad=hidden_grad, gate_weight=gate_weight, up_weight=up_weight, gate_taps=gate_taps, up_taps=up_taps, gate_bias=gate_bias, up_bias=up_bias)


def causal_mix(signal, tap_weights):
    tap_count = tap_weights.shape[0]
    length = signal.shape[0]
    padded = jnp.pad(signal, ((tap_count - 1, 0), (0, 0)))
    mixed = padded[0:length] * tap_weights[0]
    for offset in range(1, tap_count):
        mixed = mixed + padded[offset:offset + length] * tap_weights[offset]
    return mixed


def mix_back(signal, tap_weights):
    tap_count = tap_weights.shape[0]
    length = signal.shape[0]
    padded = jnp.pad(signal, ((0, tap_count - 1), (0, 0)))
    begin = tap_count - 1
    mixed = padded[begin:begin + length] * tap_weights[0]
    for offset in range(1, tap_count):
        begin = tap_count - 1 - offset
        mixed = mixed + padded[begin:begin + length] * tap_weights[offset]
    return mixed


def tap_terms(grad_signal, signal, tap_count):
    length = signal.shape[0]
    padded = jnp.pad(signal, ((tap_count - 1, 0), (0, 0)))
    return jnp.stack([jnp.sum(grad_signal * padded[offset:offset + length], axis=0) for offset in range(tap_count)])


def backward_terms(gate_pre, up_pre, hidden_grad, gate_taps, up_taps, gate_bias, up_bias):
    gate_float = gate_pre.astype(jnp.float32)
    up_float = up_pre.astype(jnp.float32)
    gate_mixed = causal_mix(gate_float, gate_taps) + gate_bias
    up_mixed = causal_mix(up_float, up_taps) + up_bias
    logistic = jax.nn.sigmoid(gate_mixed)
    cotangent = hidden_grad.astype(jnp.float32)
    gate_delta = cotangent * up_mixed * logistic * (1.0 + gate_mixed * (1.0 - logistic))
    up_delta = cotangent * gate_mixed * logistic
    gate_back = mix_back(gate_delta, gate_taps).astype(jnp.bfloat16)
    up_back = mix_back(up_delta, up_taps).astype(jnp.bfloat16)
    tap_count = gate_taps.shape[0]
    return (gate_back, up_back, tap_terms(gate_delta, gate_float, tap_count),
            tap_terms(up_delta, up_float, tap_count), jnp.sum(gate_delta, axis=0), jnp.sum(up_delta, axis=0))


def reference(tokens, gate_pre, up_pre, hidden_grad, gate_weight, up_weight, gate_taps, up_taps, gate_bias, up_bias):
    seq_shape = (N_REP, SEQ_LEN, FF)

    def per_sequence(packed):
        return backward_terms(packed[0], packed[1], packed[2], gate_taps, up_taps, gate_bias, up_bias)

    seq_parts = lax.map(per_sequence, (gate_pre.reshape(seq_shape), up_pre.reshape(seq_shape), hidden_grad.reshape(seq_shape)))
    gate_back = seq_parts[0].reshape(TOKENS, FF)
    up_back = seq_parts[1].reshape(TOKENS, FF)
    block_width = FF // N_TP

    def add_block(total, block_index):
        start = (block_index * block_width).astype(jnp.int32)
        gate_cols = lax.dynamic_slice_in_dim(gate_back, start, block_width, 1)
        up_cols = lax.dynamic_slice_in_dim(up_back, start, block_width, 1)
        gate_rows = lax.dynamic_slice_in_dim(gate_weight, start, block_width, 1)
        up_rows = lax.dynamic_slice_in_dim(up_weight, start, block_width, 1)
        block_term = (jnp.dot(gate_cols, gate_rows.T, preferred_element_type=jnp.float32)
                      + jnp.dot(up_cols, up_rows.T, preferred_element_type=jnp.float32)).astype(jnp.bfloat16)
        return total + block_term.astype(jnp.float32), None

    summed, _ = lax.scan(add_block, jnp.zeros((TOKENS, D), jnp.float32), jnp.arange(N_TP, dtype=jnp.int32))
    input_grad = summed.astype(jnp.bfloat16)
    gate_weight_grad = jnp.dot(tokens.T, gate_back, preferred_element_type=jnp.float32)
    up_weight_grad = jnp.dot(tokens.T, up_back, preferred_element_type=jnp.float32)
    return (input_grad, gate_weight_grad, up_weight_grad, jnp.sum(seq_parts[2], axis=0),
            jnp.sum(seq_parts[3], axis=0), jnp.sum(seq_parts[4], axis=0), jnp.sum(seq_parts[5], axis=0))
```

```python
import functools

import jax
import jax.numpy as jnp
from jax import lax
from jax.experimental import pallas as pl
from jax.experimental.pallas import tpu as pltpu
from jax.sharding import PartitionSpec as P

MESH = pl.DeviceIdType.MESH
CW = 128
NQ = 4
PAD = 8
F32 = jnp.float32
BF16 = jnp.bfloat16


def schedule(blocks, rep_count):
    warm = min(3, blocks)
    done = warm + (blocks - warm + 1) // 2
    steps = max(blocks + rep_count - 1, done + rep_count, done + 3)
    return warm, done, steps


def fused(
    rep_count,
    tp_count,
    tokens,
    gate_pre,
    up_pre,
    hidden,
    gate_weight,
    up_weight,
    gate_taps,
    up_taps,
    gate_bias,
    up_bias,
    grad_out,
    gate_out,
    up_out,
    small_out,
    tok,
    tok_t,
    gpre,
    upre,
    hid,
    gw,
    uw,
    gpad,
    upad,
    gdel,
    udel,
    back,
    acc,
    own,
    from_left,
    from_right,
    to_right,
    to_left,
    out_stage,
    term,
    term_in,
    final,
    small,
    small_from_left,
    small_from_right,
    small_to_right,
    small_to_left,
    load_sem,
    weight_sem,
    send_r,
    recv_r,
    send_l,
    recv_l,
    out_sem,
    scatter_send,
    scatter_recv,
    gather_send,
    gather_recv,
    final_sem,
    small_sem,
):
    z = lax.axis_index("rep")
    me = lax.axis_index("tp")
    length, hidden_cols = gate_pre.shape
    width = tokens.shape[1]
    blocks = hidden_cols // CW
    rows_q = width // NQ
    taps = gate_taps.shape[0]
    warm, done, steps = schedule(blocks, rep_count)
    has_left = z > 0
    has_right = z < rep_count - 1

    def columns(b):
        return pl.ds(pl.multiple_of(b * CW, CW), CW)

    def load(which, b):
        src = (gate_pre, up_pre, hidden)[which]
        dst = (gpre, upre, hid)[which]
        return pltpu.make_async_copy(
            src.at[:, columns(b)], dst.at[b], load_sem.at[which, b]
        )

    token_copy = pltpu.make_async_copy(tokens, tok, weight_sem.at[0])
    weight_copies = (
        pltpu.make_async_copy(gate_weight, gw, weight_sem.at[1]),
        pltpu.make_async_copy(up_weight, uw, weight_sem.at[2]),
    )
    for which in range(3):
        load(which, 0).start()
    token_copy.start()

    def start_load(b, carry):
        for which in range(3):
            load(which, b).start()
        return carry

    lax.fori_loop(1, blocks, start_load, 0)
    for copy in weight_copies:
        copy.start()

    barrier = pltpu.get_barrier_semaphore()

    @pl.when(has_left)
    def _():
        pl.semaphore_signal(barrier, inc=1, device_id={"rep": z - 1}, device_id_type=MESH)

    @pl.when(has_right)
    def _():
        pl.semaphore_signal(barrier, inc=1, device_id={"rep": z + 1}, device_id_type=MESH)

    for d in range(1, tp_count):
        peer = lax.rem(me + d, tp_count)
        pl.semaphore_signal(barrier, inc=1, device_id={"tp": peer}, device_id_type=MESH)

    @pl.when(z == 0)
    def _():
        small_from_left[...] = jnp.zeros_like(small_from_left)

        def clear(c, carry):
            from_left[c] = jnp.zeros((rows_q, 2 * CW), BF16)
            return carry

        lax.fori_loop(0, blocks * NQ, clear, 0)

    @pl.when(z == rep_count - 1)
    def _():
        small_from_right[...] = jnp.zeros_like(small_from_right)

        def clear(c, carry):
            from_right[c] = jnp.zeros((rows_q, 2 * CW), BF16)
            return carry

        lax.fori_loop(0, blocks * NQ, clear, 0)

    zero_rows = jnp.zeros((PAD, CW), F32)
    gpad[0:PAD, :] = zero_rows
    upad[0:PAD, :] = zero_rows
    gdel[length : length + PAD, :] = zero_rows
    udel[length : length + PAD, :] = zero_rows
    acc[...] = jnp.zeros_like(acc)

    token_copy.wait()
    for i in range(width // CW):
        tok_t[i * CW : (i + 1) * CW, :] = tok[:, i * CW : (i + 1) * CW].T

    pl.semaphore_wait(
        barrier,
        jnp.where(has_left, 1, 0) + jnp.where(has_right, 1, 0) + (tp_count - 1),
    )

    row_tile = 128 if length % 128 == 0 else length

    def folded(x):
        return jnp.sum(x.reshape(x.shape[0] // 8, 8, CW), axis=0)

    def compute(b, carry):
        for which in range(3):
            load(which, b).wait()
        cols = columns(b)
        gt = [gate_taps[k : k + 1, cols] for k in range(taps)]
        ut = [up_taps[k : k + 1, cols] for k in range(taps)]
        gb = gate_bias[:, cols]
        ub = up_bias[:, cols]
        for r in range(0, length, row_tile):
            gpad[PAD + r : PAD + r + row_tile, :] = gpre[b, r : r + row_tile, :].astype(F32)
            upad[PAD + r : PAD + r + row_tile, :] = upre[b, r : r + row_tile, :].astype(F32)
        sums = None
        for r in range(0, length, row_tile):
            start = PAD + r - (taps - 1)
            gs = [gpad[start + k : start + k + row_tile, :] for k in range(taps)]
            us = [upad[start + k : start + k + row_tile, :] for k in range(taps)]
            gm = gs[0] * gt[0]
            um = us[0] * ut[0]
            for k in range(1, taps):
                gm = gm + gs[k] * gt[k]
                um = um + us[k] * ut[k]
            gm = gm + gb
            um = um + ub
            s = jax.nn.sigmoid(gm)
            h = hid[b, r : r + row_tile, :].astype(F32)
            gd = h * um * s * (1.0 + gm * (1.0 - s))
            ud = h * gm * s
            gdel[r : r + row_tile, :] = gd
            udel[r : r + row_tile, :] = ud
            parts = (
                [folded(gd * g) for g in gs]
                + [folded(ud * u) for u in us]
                + [folded(gd), folded(ud)]
            )
            sums = parts if sums is None else [a + p for a, p in zip(sums, parts)]
        for k, part in enumerate(sums):
            small[k : k + 1, cols] = jnp.sum(part, axis=0, keepdims=True)
        for r in range(0, length, row_tile):
            first = r + taps - 1
            gk = gdel[first : first + row_tile, :] * gt[0]
            uk = udel[first : first + row_tile, :] * ut[0]
            for k in range(1, taps):
                first = r + taps - 1 - k
                gk = gk + gdel[first : first + row_tile, :] * gt[k]
                uk = uk + udel[first : first + row_tile, :] * ut[k]
            back[r : r + row_tile, 0:CW] = gk.astype(BF16)
            back[r : r + row_tile, CW : 2 * CW] = uk.astype(BF16)
        block = back[...]
        for q in range(NQ):
            own[b * NQ + q] = jnp.dot(
                tok_t[q * rows_q : (q + 1) * rows_q, :], block, preferred_element_type=F32
            ).astype(BF16)

        @pl.when(b == 0)
        def _():
            for copy in weight_copies:
                copy.wait()

        weights = jnp.concatenate([gw[:, cols], uw[:, cols]], axis=1)
        dot_rows = 256 if length % 256 == 0 else length
        for r in range(0, length, dot_rows):
            acc[r : r + dot_rows, :] += lax.dot_general(
                back[r : r + dot_rows, :],
                weights,
                (((1,), (1,)), ((), ())),
                preferred_element_type=F32,
            )
        return carry

    def right_copy(c):
        return pltpu.make_async_remote_copy(
            src_ref=to_right.at[c],
            dst_ref=from_left.at[c],
            send_sem=send_r.at[c],
            recv_sem=recv_r.at[c],
            device_id={"rep": z + 1},
            device_id_type=MESH,
        )

    def left_copy(c):
        return pltpu.make_async_remote_copy(
            src_ref=to_left.at[c],
            dst_ref=from_right.at[c],
            send_sem=send_l.at[c],
            recv_sem=recv_l.at[c],
            device_id={"rep": z - 1},
            device_id_type=MESH,
        )

    small_right = pltpu.make_async_remote_copy(
        src_ref=small_to_right,
        dst_ref=small_from_left,
        send_sem=small_sem.at[0],
        recv_sem=small_sem.at[1],
        device_id={"rep": z + 1},
        device_id_type=MESH,
    )
    small_left = pltpu.make_async_remote_copy(
        src_ref=small_to_left,
        dst_ref=small_from_right,
        send_sem=small_sem.at[2],
        recv_sem=small_sem.at[3],
        device_id={"rep": z - 1},
        device_id_type=MESH,
    )

    def out_copies(b, q):
        rows = pl.ds(q * rows_q, rows_q)
        return (
            pltpu.make_async_copy(
                out_stage.at[0, q], gate_out.at[rows, columns(b)], out_sem.at[0, q]
            ),
            pltpu.make_async_copy(
                out_stage.at[1, q], up_out.at[rows, columns(b)], out_sem.at[1, q]
            ),
        )

    def scatter_copy(d):
        peer = lax.rem(me + d, tp_count)
        return pltpu.make_async_remote_copy(
            src_ref=term.at[peer],
            dst_ref=term_in.at[d - 1],
            send_sem=scatter_send.at[d - 1],
            recv_sem=scatter_recv.at[d - 1],
            device_id={"tp": peer},
            device_id_type=MESH,
        )

    def gather_copy(d, slot):
        return pltpu.make_async_remote_copy(
            src_ref=final.at[slot],
            dst_ref=final.at[slot],
            send_sem=gather_send.at[d - 1],
            recv_sem=gather_recv.at[d - 1],
            device_id={"tp": lax.rem(me + d, tp_count)},
            device_id_type=MESH,
        )

    term_rows = length // tp_count

    def step(s, carry):
        first = jnp.where(s < warm, s, 2 * s - warm)
        last = jnp.minimum(jnp.where(s < warm, s + 1, 2 * s - warm + 2), blocks)
        lax.fori_loop(first, last, compute, 0)

        b_right = s - z
        b_left = s - (rep_count - 1 - z)
        b_out = s - (rep_count - 1)
        for q in range(NQ):

            @pl.when((b_right >= 0) & (b_right < blocks))
            def _():
                c = b_right * NQ + q

                @pl.when(has_left)
                def _():
                    right_copy(c).wait_recv()

                @pl.when(has_right)
                def _():
                    to_right[c] = (from_left[c].astype(F32) + own[c].astype(F32)).astype(BF16)
                    right_copy(c).start()

            @pl.when((b_left >= 0) & (b_left < blocks))
            def _():
                c = b_left * NQ + q

                @pl.when(has_right)
                def _():
                    left_copy(c).wait_recv()

                @pl.when(has_left)
                def _():
                    to_left[c] = (from_right[c].astype(F32) + own[c].astype(F32)).astype(BF16)
                    left_copy(c).start()

            @pl.when((b_out >= 0) & (b_out < blocks))
            def _():
                c = b_out * NQ + q

                @pl.when(b_out > 0)
                def _():
                    for copy in out_copies(b_out - 1, q):
                        copy.wait()

                total = (
                    from_left[c].astype(F32) + own[c].astype(F32) + from_right[c].astype(F32)
                ).astype(BF16)
                out_stage[0, q] = total[:, 0:CW]
                out_stage[1, q] = total[:, CW : 2 * CW]
                for copy in out_copies(b_out, q):
                    copy.start()

        @pl.when(s == done)
        def _():
            for k in range(tp_count):
                term[k] = acc[k * term_rows : (k + 1) * term_rows, :].astype(BF16)
            for d in range(1, tp_count):
                scatter_copy(d).start()

        @pl.when(s == done + 2)
        def _():
            total = term[me].astype(F32)
            for d in range(1, tp_count):
                scatter_copy(d).wait()
                total = total + term_in[d - 1].astype(F32)
            final[me] = total.astype(BF16)
            for d in range(1, tp_count):
                gather_copy(d, me).start()

        @pl.when(s == done + z)
        def _():
            @pl.when(has_left)
            def _():
                small_right.wait_recv()

            @pl.when(has_right)
            def _():
                small_to_right[...] = small_from_left[...] + small[...]
                small_right.start()

        @pl.when(s == done + rep_count - 1 - z)
        def _():
            @pl.when(has_right)
            def _():
                small_left.wait_recv()

            @pl.when(has_left)
            def _():
                small_to_left[...] = small_from_right[...] + small[...]
                small_left.start()

        return carry

    lax.fori_loop(0, steps, step, 0)

    def final_copy(slot):
        return pltpu.make_async_copy(
            final.at[slot],
            grad_out.at[pl.ds(pl.multiple_of(slot * term_rows, term_rows), term_rows), :],
            final_sem.at[slot],
        )

    final_copy(me).start()
    for d in range(1, tp_count):
        sender = lax.rem(me + tp_count - d, tp_count)
        gather_copy(d, sender).wait_recv()
        final_copy(sender).start()
    for d in range(1, tp_count):
        gather_copy(d, me).wait_send()
    small_out[...] = small_from_left[...] + small[...] + small_from_right[...]

    @pl.when(has_right)
    def _():
        small_right.wait_send()

        def drain(c, carry):
            right_copy(c).wait_send()
            return carry

        lax.fori_loop(0, blocks * NQ, drain, 0)

    @pl.when(has_left)
    def _():
        small_left.wait_send()

        def drain(c, carry):
            left_copy(c).wait_send()
            return carry

        lax.fori_loop(0, blocks * NQ, drain, 0)

    for q in range(NQ):
        for copy in out_copies(blocks - 1, q):
            copy.wait()
    for slot in range(tp_count):
        final_copy(slot).wait()


def per_device(
    rep_count,
    tp_count,
    tokens,
    gate_pre,
    up_pre,
    hidden_grad,
    gate_weight,
    up_weight,
    gate_taps,
    up_taps,
    gate_bias,
    up_bias,
):
    length, hidden_cols = gate_pre.shape
    width = tokens.shape[1]
    taps = gate_taps.shape[0]
    blocks = hidden_cols // CW
    chunks = blocks * NQ
    rows_q = width // NQ
    term_rows = length // tp_count
    small_rows = 2 * taps + 2
    anywhere = pl.BlockSpec(memory_space=pl.ANY)
    vmem = pl.BlockSpec(memory_space=pltpu.VMEM)
    line = pltpu.VMEM((chunks, rows_q, 2 * CW), BF16)
    small = pltpu.VMEM((small_rows, hidden_cols), F32)
    dma = pltpu.SemaphoreType.DMA
    grad, gate_sum, up_sum, small_sum = pl.pallas_call(
        functools.partial(fused, rep_count, tp_count),
        out_shape=(
            jax.ShapeDtypeStruct((length, width), BF16),
            jax.ShapeDtypeStruct((width, hidden_cols), BF16),
            jax.ShapeDtypeStruct((width, hidden_cols), BF16),
            jax.ShapeDtypeStruct((small_rows, hidden_cols), F32),
        ),
        in_specs=[anywhere] * 6 + [vmem] * 4,
        out_specs=(anywhere, anywhere, anywhere, vmem),
        scratch_shapes=[
            pltpu.VMEM((length, width), BF16),
            pltpu.VMEM((width, length), BF16),
            pltpu.VMEM((blocks, length, CW), BF16),
            pltpu.VMEM((blocks, length, CW), BF16),
            pltpu.VMEM((blocks, length, CW), BF16),
            pltpu.VMEM((width, hidden_cols), BF16),
            pltpu.VMEM((width, hidden_cols), BF16),
            pltpu.VMEM((PAD + length, CW), F32),
            pltpu.VMEM((PAD + length, CW), F32),
            pltpu.VMEM((length + PAD, CW), F32),
            pltpu.VMEM((length + PAD, CW), F32),
            pltpu.VMEM((length, 2 * CW), BF16),
            pltpu.VMEM((length, width), F32),
            line,
            line,
            line,
            line,
            line,
            pltpu.VMEM((2, NQ, rows_q, CW), BF16),
            pltpu.VMEM((tp_count, term_rows, width), BF16),
            pltpu.VMEM((tp_count - 1, term_rows, width), BF16),
            pltpu.VMEM((tp_count, term_rows, width), BF16),
            small,
            small,
            small,
            small,
            small,
            dma((3, blocks)),
            dma((3,)),
            dma((chunks,)),
            dma((chunks,)),
            dma((chunks,)),
            dma((chunks,)),
            dma((2, NQ)),
            dma((tp_count - 1,)),
            dma((tp_count - 1,)),
            dma((tp_count - 1,)),
            dma((tp_count - 1,)),
            dma((tp_count,)),
            dma((4,)),
        ],
        compiler_params=pltpu.CompilerParams(
            collective_id=0, has_side_effects=True, vmem_limit_bytes=67043328
        ),
    )(
        tokens,
        gate_pre,
        up_pre,
        hidden_grad,
        gate_weight,
        up_weight,
        gate_taps,
        up_taps,
        gate_bias[None, :],
        up_bias[None, :],
    )
    return (
        grad,
        gate_sum.astype(F32),
        up_sum.astype(F32),
        small_sum[0:taps],
        small_sum[taps : 2 * taps],
        small_sum[2 * taps],
        small_sum[2 * taps + 1],
    )


def solution(mesh):
    return jax.shard_map(
        functools.partial(per_device, mesh.shape["rep"], mesh.shape["tp"]),
        mesh=mesh,
        in_specs=(
            P("rep", "fs"),
            P("rep", "tp"),
            P("rep", "tp"),
            P("rep", "tp"),
            P("fs", "tp"),
            P("fs", "tp"),
            P(None, "tp"),
            P(None, "tp"),
            P("tp"),
            P("tp"),
        ),
        out_specs=(
            P("rep", "fs"),
            P("fs", "tp"),
            P("fs", "tp"),
            P(None, "tp"),
            P(None, "tp"),
            P("tp"),
            P("tp"),
        ),
        check_vma=False,
    )
```

```python
import functools

import jax
import jax.numpy as jnp
from jax import lax
from jax.experimental import pallas as pl
from jax.experimental.pallas import tpu as pltpu
from jax.sharding import PartitionSpec as P

MESH = pl.DeviceIdType.MESH
CW = 128
NQ = 8
PAD = 8
F32 = jnp.float32
BF16 = jnp.bfloat16


def schedule(blocks, rep_count):
    warm = min(3, blocks)
    done = warm + (blocks - warm + 1) // 2
    steps = max(blocks + rep_count - 1, done + rep_count, done + 3)
    return warm, done, steps


def fused(
    rep_count,
    tp_count,
    tokens,
    gate_pre,
    up_pre,
    hidden,
    gate_weight,
    up_weight,
    gate_taps,
    up_taps,
    gate_bias,
    up_bias,
    grad_out,
    gate_out,
    up_out,
    small_out,
    tok,
    tok_t,
    gpre,
    upre,
    hid,
    gw,
    uw,
    gpad,
    upad,
    gdel,
    udel,
    back,
    acc,
    own,
    from_left,
    from_right,
    to_right,
    to_left,
    out_stage,
    term,
    term_in,
    final,
    small,
    small_from_left,
    small_from_right,
    small_to_right,
    small_to_left,
    load_sem,
    weight_sem,
    send_r,
    recv_r,
    send_l,
    recv_l,
    out_sem,
    scatter_send,
    scatter_recv,
    gather_send,
    gather_recv,
    final_sem,
    small_sem,
):
    z = lax.axis_index("rep")
    me = lax.axis_index("tp")
    length, hidden_cols = gate_pre.shape
    width = tokens.shape[1]
    blocks = hidden_cols // CW
    rows_q = width // NQ
    taps = gate_taps.shape[0]
    warm, done, steps = schedule(blocks, rep_count)
    has_left = z > 0
    has_right = z < rep_count - 1

    def columns(b):
        return pl.ds(pl.multiple_of(b * CW, CW), CW)

    def load(which, b):
        src = (gate_pre, up_pre, hidden)[which]
        dst = (gpre, upre, hid)[which]
        return pltpu.make_async_copy(
            src.at[:, columns(b)], dst.at[b], load_sem.at[which, b]
        )

    token_copy = pltpu.make_async_copy(tokens, tok, weight_sem.at[0])
    weight_copies = (
        pltpu.make_async_copy(gate_weight, gw, weight_sem.at[1]),
        pltpu.make_async_copy(up_weight, uw, weight_sem.at[2]),
    )
    for which in range(3):
        load(which, 0).start()
    token_copy.start()

    def start_load(b, carry):
        for which in range(3):
            load(which, b).start()
        return carry

    lax.fori_loop(1, blocks, start_load, 0)
    for copy in weight_copies:
        copy.start()

    barrier = pltpu.get_barrier_semaphore()

    @pl.when(has_left)
    def _():
        pl.semaphore_signal(barrier, inc=1, device_id={"rep": z - 1}, device_id_type=MESH)

    @pl.when(has_right)
    def _():
        pl.semaphore_signal(barrier, inc=1, device_id={"rep": z + 1}, device_id_type=MESH)

    for d in range(1, tp_count):
        peer = lax.rem(me + d, tp_count)
        pl.semaphore_signal(barrier, inc=1, device_id={"tp": peer}, device_id_type=MESH)

    @pl.when(z == 0)
    def _():
        small_from_left[...] = jnp.zeros_like(small_from_left)

        def clear(c, carry):
            from_left[c] = jnp.zeros((rows_q, 2 * CW), BF16)
            return carry

        lax.fori_loop(0, blocks * NQ, clear, 0)

    @pl.when(z == rep_count - 1)
    def _():
        small_from_right[...] = jnp.zeros_like(small_from_right)

        def clear(c, carry):
            from_right[c] = jnp.zeros((rows_q, 2 * CW), BF16)
            return carry

        lax.fori_loop(0, blocks * NQ, clear, 0)

    zero_rows = jnp.zeros((PAD, CW), F32)
    gpad[0:PAD, :] = zero_rows
    upad[0:PAD, :] = zero_rows
    gdel[length : length + PAD, :] = zero_rows
    udel[length : length + PAD, :] = zero_rows
    acc[...] = jnp.zeros_like(acc)

    token_copy.wait()
    for i in range(width // CW):
        tok_t[i * CW : (i + 1) * CW, :] = tok[:, i * CW : (i + 1) * CW].T

    pl.semaphore_wait(
        barrier,
        jnp.where(has_left, 1, 0) + jnp.where(has_right, 1, 0) + (tp_count - 1),
    )

    row_tile = 128 if length % 128 == 0 else length

    def folded(x):
        return jnp.sum(x.reshape(x.shape[0] // 8, 8, CW), axis=0)

    def compute(b, carry):
        for which in range(3):
            load(which, b).wait()
        cols = columns(b)
        gt = [gate_taps[k : k + 1, cols] for k in range(taps)]
        ut = [up_taps[k : k + 1, cols] for k in range(taps)]
        gb = gate_bias[cols].reshape(1, CW)
        ub = up_bias[cols].reshape(1, CW)
        for r in range(0, length, row_tile):
            gpad[PAD + r : PAD + r + row_tile, :] = gpre[b, r : r + row_tile, :].astype(F32)
            upad[PAD + r : PAD + r + row_tile, :] = upre[b, r : r + row_tile, :].astype(F32)
        sums = None
        for r in range(0, length, row_tile):
            start = PAD + r - (taps - 1)
            gs = [gpad[start + k : start + k + row_tile, :] for k in range(taps)]
            us = [upad[start + k : start + k + row_tile, :] for k in range(taps)]
            gm = gs[0] * gt[0]
            um = us[0] * ut[0]
            for k in range(1, taps):
                gm = gm + gs[k] * gt[k]
                um = um + us[k] * ut[k]
            gm = gm + gb
            um = um + ub
            s = jax.nn.sigmoid(gm)
            h = hid[b, r : r + row_tile, :].astype(F32)
            gd = h * um * s * (1.0 + gm * (1.0 - s))
            ud = h * gm * s
            gdel[r : r + row_tile, :] = gd
            udel[r : r + row_tile, :] = ud
            parts = (
                [folded(gd * g) for g in gs]
                + [folded(ud * u) for u in us]
                + [folded(gd), folded(ud)]
            )
            sums = parts if sums is None else [a + p for a, p in zip(sums, parts)]
        for k, part in enumerate(sums):
            small[k : k + 1, cols] = jnp.sum(part, axis=0, keepdims=True)
        for r in range(0, length, row_tile):
            first = r + taps - 1
            gk = gdel[first : first + row_tile, :] * gt[0]
            uk = udel[first : first + row_tile, :] * ut[0]
            for k in range(1, taps):
                first = r + taps - 1 - k
                gk = gk + gdel[first : first + row_tile, :] * gt[k]
                uk = uk + udel[first : first + row_tile, :] * ut[k]
            back[r : r + row_tile, 0:CW] = gk.astype(BF16)
            back[r : r + row_tile, CW : 2 * CW] = uk.astype(BF16)
        block = back[...]
        for q in range(NQ):
            own[b * NQ + q] = jnp.dot(
                tok_t[q * rows_q : (q + 1) * rows_q, :], block, preferred_element_type=F32
            ).astype(BF16)

        @pl.when(b == 0)
        def _():
            for copy in weight_copies:
                copy.wait()

        weights = jnp.concatenate([gw[:, cols], uw[:, cols]], axis=1)
        dot_rows = 256 if length % 256 == 0 else length
        for r in range(0, length, dot_rows):
            acc[r : r + dot_rows, :] += lax.dot_general(
                back[r : r + dot_rows, :],
                weights,
                (((1,), (1,)), ((), ())),
                preferred_element_type=F32,
            )
        return carry

    def right_copy(c):
        return pltpu.make_async_remote_copy(
            src_ref=to_right.at[c],
            dst_ref=from_left.at[c],
            send_sem=send_r.at[c],
            recv_sem=recv_r.at[c],
            device_id={"rep": z + 1},
            device_id_type=MESH,
        )

    def left_copy(c):
        return pltpu.make_async_remote_copy(
            src_ref=to_left.at[c],
            dst_ref=from_right.at[c],
            send_sem=send_l.at[c],
            recv_sem=recv_l.at[c],
            device_id={"rep": z - 1},
            device_id_type=MESH,
        )

    small_right = pltpu.make_async_remote_copy(
        src_ref=small_to_right,
        dst_ref=small_from_left,
        send_sem=small_sem.at[0],
        recv_sem=small_sem.at[1],
        device_id={"rep": z + 1},
        device_id_type=MESH,
    )
    small_left = pltpu.make_async_remote_copy(
        src_ref=small_to_left,
        dst_ref=small_from_right,
        send_sem=small_sem.at[2],
        recv_sem=small_sem.at[3],
        device_id={"rep": z - 1},
        device_id_type=MESH,
    )

    def out_copies(b, q):
        rows = pl.ds(q * rows_q, rows_q)
        return (
            pltpu.make_async_copy(
                out_stage.at[0, q], gate_out.at[rows, columns(b)], out_sem.at[0, q]
            ),
            pltpu.make_async_copy(
                out_stage.at[1, q], up_out.at[rows, columns(b)], out_sem.at[1, q]
            ),
        )

    def scatter_copy(d):
        peer = lax.rem(me + d, tp_count)
        return pltpu.make_async_remote_copy(
            src_ref=term.at[peer],
            dst_ref=term_in.at[d - 1],
            send_sem=scatter_send.at[d - 1],
            recv_sem=scatter_recv.at[d - 1],
            device_id={"tp": peer},
            device_id_type=MESH,
        )

    def gather_copy(d, slot):
        return pltpu.make_async_remote_copy(
            src_ref=final.at[slot],
            dst_ref=final.at[slot],
            send_sem=gather_send.at[d - 1],
            recv_sem=gather_recv.at[d - 1],
            device_id={"tp": lax.rem(me + d, tp_count)},
            device_id_type=MESH,
        )

    term_rows = length // tp_count

    def step(s, carry):
        first = jnp.where(s < warm, s, 2 * s - warm)
        last = jnp.minimum(jnp.where(s < warm, s + 1, 2 * s - warm + 2), blocks)
        lax.fori_loop(first, last, compute, 0)

        b_right = s - z
        b_left = s - (rep_count - 1 - z)
        b_out = s - (rep_count - 1)
        for q in range(NQ):

            @pl.when((b_right >= 0) & (b_right < blocks))
            def _():
                c = b_right * NQ + q

                @pl.when(has_left)
                def _():
                    right_copy(c).wait_recv()

                @pl.when(has_right)
                def _():
                    to_right[c] = (from_left[c].astype(F32) + own[c].astype(F32)).astype(BF16)
                    right_copy(c).start()

            @pl.when((b_left >= 0) & (b_left < blocks))
            def _():
                c = b_left * NQ + q

                @pl.when(has_right)
                def _():
                    left_copy(c).wait_recv()

                @pl.when(has_left)
                def _():
                    to_left[c] = (from_right[c].astype(F32) + own[c].astype(F32)).astype(BF16)
                    left_copy(c).start()

            @pl.when((b_out >= 0) & (b_out < blocks))
            def _():
                c = b_out * NQ + q

                @pl.when(b_out > 0)
                def _():
                    for copy in out_copies(b_out - 1, q):
                        copy.wait()

                total = (
                    from_left[c].astype(F32) + own[c].astype(F32) + from_right[c].astype(F32)
                ).astype(BF16)
                out_stage[0, q] = total[:, 0:CW]
                out_stage[1, q] = total[:, CW : 2 * CW]
                for copy in out_copies(b_out, q):
                    copy.start()

        @pl.when(s == done)
        def _():
            for k in range(tp_count):
                term[k] = acc[k * term_rows : (k + 1) * term_rows, :].astype(BF16)
            for d in range(1, tp_count):
                scatter_copy(d).start()

        @pl.when(s == done + 2)
        def _():
            total = term[me].astype(F32)
            for d in range(1, tp_count):
                scatter_copy(d).wait()
                total = total + term_in[d - 1].astype(F32)
            final[me] = total.astype(BF16)
            for d in range(1, tp_count):
                gather_copy(d, me).start()

        @pl.when(s == done + z)
        def _():
            @pl.when(has_left)
            def _():
                small_right.wait_recv()

            @pl.when(has_right)
            def _():
                small_to_right[...] = small_from_left[...] + small[...]
                small_right.start()

        @pl.when(s == done + rep_count - 1 - z)
        def _():
            @pl.when(has_right)
            def _():
                small_left.wait_recv()

            @pl.when(has_left)
            def _():
                small_to_left[...] = small_from_right[...] + small[...]
                small_left.start()

        return carry

    lax.fori_loop(0, steps, step, 0)

    def final_copy(slot):
        return pltpu.make_async_copy(
            final.at[slot],
            grad_out.at[pl.ds(pl.multiple_of(slot * term_rows, term_rows), term_rows), :],
            final_sem.at[slot],
        )

    final_copy(me).start()
    for d in range(1, tp_count):
        sender = lax.rem(me + tp_count - d, tp_count)
        gather_copy(d, sender).wait_recv()
        final_copy(sender).start()
    for d in range(1, tp_count):
        gather_copy(d, me).wait_send()
    small_out[...] = small_from_left[...] + small[...] + small_from_right[...]

    @pl.when(has_right)
    def _():
        small_right.wait_send()

        def drain(c, carry):
            right_copy(c).wait_send()
            return carry

        lax.fori_loop(0, blocks * NQ, drain, 0)

    @pl.when(has_left)
    def _():
        small_left.wait_send()

        def drain(c, carry):
            left_copy(c).wait_send()
            return carry

        lax.fori_loop(0, blocks * NQ, drain, 0)

    for q in range(NQ):
        for copy in out_copies(blocks - 1, q):
            copy.wait()
    for slot in range(tp_count):
        final_copy(slot).wait()


def per_device(
    rep_count,
    tp_count,
    tokens,
    gate_pre,
    up_pre,
    hidden_grad,
    gate_weight,
    up_weight,
    gate_taps,
    up_taps,
    gate_bias,
    up_bias,
):
    length, hidden_cols = gate_pre.shape
    width = tokens.shape[1]
    taps = gate_taps.shape[0]
    blocks = hidden_cols // CW
    chunks = blocks * NQ
    rows_q = width // NQ
    term_rows = length // tp_count
    small_rows = 2 * taps + 2
    anywhere = pl.BlockSpec(memory_space=pl.ANY)
    vmem = pl.BlockSpec(memory_space=pltpu.VMEM)
    line = pltpu.VMEM((chunks, rows_q, 2 * CW), BF16)
    small = pltpu.VMEM((small_rows, hidden_cols), F32)
    dma = pltpu.SemaphoreType.DMA
    grad, gate_sum, up_sum, small_sum = pl.pallas_call(
        functools.partial(fused, rep_count, tp_count),
        out_shape=(
            jax.ShapeDtypeStruct((length, width), BF16),
            jax.ShapeDtypeStruct((width, hidden_cols), BF16),
            jax.ShapeDtypeStruct((width, hidden_cols), BF16),
            jax.ShapeDtypeStruct((small_rows, hidden_cols), F32),
        ),
        in_specs=[anywhere] * 6 + [vmem] * 4,
        out_specs=(anywhere, anywhere, anywhere, vmem),
        scratch_shapes=[
            pltpu.VMEM((length, width), BF16),
            pltpu.VMEM((width, length), BF16),
            pltpu.VMEM((blocks, length, CW), BF16),
            pltpu.VMEM((blocks, length, CW), BF16),
            pltpu.VMEM((blocks, length, CW), BF16),
            pltpu.VMEM((width, hidden_cols), BF16),
            pltpu.VMEM((width, hidden_cols), BF16),
            pltpu.VMEM((PAD + length, CW), F32),
            pltpu.VMEM((PAD + length, CW), F32),
            pltpu.VMEM((length + PAD, CW), F32),
            pltpu.VMEM((length + PAD, CW), F32),
            pltpu.VMEM((length, 2 * CW), BF16),
            pltpu.VMEM((length, width), F32),
            line,
            line,
            line,
            line,
            line,
            pltpu.VMEM((2, NQ, rows_q, CW), BF16),
            pltpu.VMEM((tp_count, term_rows, width), BF16),
            pltpu.VMEM((tp_count - 1, term_rows, width), BF16),
            pltpu.VMEM((tp_count, term_rows, width), BF16),
            small,
            small,
            small,
            small,
            small,
            dma((3, blocks)),
            dma((3,)),
            dma((chunks,)),
            dma((chunks,)),
            dma((chunks,)),
            dma((chunks,)),
            dma((2, NQ)),
            dma((tp_count - 1,)),
            dma((tp_count - 1,)),
            dma((tp_count - 1,)),
            dma((tp_count - 1,)),
            dma((tp_count,)),
            dma((4,)),
        ],
        compiler_params=pltpu.CompilerParams(
            collective_id=0, has_side_effects=True, vmem_limit_bytes=67043328
        ),
    )(
        tokens,
        gate_pre,
        up_pre,
        hidden_grad,
        gate_weight,
        up_weight,
        gate_taps,
        up_taps,
        gate_bias,
        up_bias,
    )
    return (
        grad,
        gate_sum.astype(F32),
        up_sum.astype(F32),
        small_sum[0:taps],
        small_sum[taps : 2 * taps],
        small_sum[2 * taps],
        small_sum[2 * taps + 1],
    )


def solution(mesh):
    return jax.shard_map(
        functools.partial(per_device, mesh.shape["rep"], mesh.shape["tp"]),
        mesh=mesh,
        in_specs=(
            P("rep", "fs"),
            P("rep", "tp"),
            P("rep", "tp"),
            P("rep", "tp"),
            P("fs", "tp"),
            P("fs", "tp"),
            P(None, "tp"),
            P(None, "tp"),
            P("tp"),
            P("tp"),
        ),
        out_specs=(
            P("rep", "fs"),
            P("fs", "tp"),
            P("fs", "tp"),
            P(None, "tp"),
            P(None, "tp"),
            P("tp"),
            P("tp"),
        ),
        check_vma=False,
    )
```
